32 devices in a mesh: grp: 2 (over y), sp: 4 (over z), tp: 4 (over x, core).
Axes of the slice: x: 2, y: 2, z: 4, core: 2. Of those that a mesh axis runs over, the one named last changes fastest.
Arguments:
- residual: bfloat16 [4096, 2048], P(('grp', 'sp')), parts along dimension 0, may hold values from -6 to 6
- values: bfloat16 [4096, 4096], P(('grp', 'sp'), 'tp'), parts along dimension 0, may hold values from -6 to 6
- out_gate: bfloat16 [4096, 4096], P(('grp', 'sp'), 'tp'), parts along dimension 0, may hold values from -6 to 6
- writes: bfloat16 [4096, 1024], P(('grp', 'sp'), 'tp'), parts along dimension 0, may hold values from -6 to 6
- reads: bfloat16 [4096, 1024], P(('grp', 'sp'), 'tp'), parts along dimension 0, may hold values from -6 to 6
- step_raw: bfloat16 [64, 4096], P('tp', ('grp', 'sp')), parts along dimension 1, may hold values from -4.5 to 4.5
- decay_rate: float32 [64], P('tp'), may hold values from 0 to 0.1
- decay_jump: float32 [64, 4096], P('tp', ('grp', 'sp')), parts along dimension 1, may hold values from -0.7 to 0
- documents: int32 [4096], P(('grp', 'sp')), parts along dimension 0, may hold values from 0 to 1, never falling along the last dimension, each value on 1 to 1536 neighbouring positions
- taps_values: bfloat16 [4, 4096], P(None, 'tp'), may hold values from -3 to 3
- taps_write: bfloat16 [4, 1024], P(None, 'tp'), may hold values from -3 to 3
- taps_read: bfloat16 [4, 1024], P(None, 'tp'), may hold values from -3 to 3
- mixer_gain: bfloat16 [4096], P('tp'), may hold values from 0.099609375 to 1.8984375
- mixer_out: bfloat16 [4096, 2048], P('tp'), may hold values from -0.09375 to 0.09375
- channel_gain: bfloat16 [2048], replicated, may hold values from 0.099609375 to 1.8984375
- gate_weight: bfloat16 [2048, 5632], P('sp', 'tp'), may hold values from -0.125 to 0.125
- up_weight: bfloat16 [2048, 5632], P('sp', 'tp'), may hold values from -0.125 to 0.125
- down_rows: bfloat16 [2048, 5632], P('sp', 'tp'), may hold values from -0.078125 to 0.078125
Outputs:
- layer_out: bfloat16 [4096, 2048], P(('grp', 'sp'), 'tp'), parts along dimension 0
The draws below stay inside these ranges and needn't reach their ends.
There are 2 independent parts, one for each index of `grp`. The reference program is written for one: setup_inputs(seed, part) draws one part's arguments, and reference() takes and returns one part's arrays. A program takes and returns all parts, laid end to end along the dimension named above; an argument that names none is the same for every part. Nothing has to cross between parts.
Inputs may be any that keep to these rules, and one draw needn't show every extreme that they name: `documents`: document numbers never fall along the sequence; a document starts where the number changes, and is one to 1536 positions long.
All inputs are finite; a program needn't handle non-finite values.
Results may differ from the reference program's by a relative error of at most 0.017.
Values may be sent and summed in bfloat16 or wider, within the bound.
A program may use at most 64 MiB of HBM per device.

```python
import math
import jax
import jax.numpy as jnp
import numpy as np
from jax import lax

D = 2048
HEADS = 64
HDIM = 64
GROUPS = 8
STATE = 128
CONV = 4
FF = 5632
BLOCK = 128
TOK_DEV = 512
SEQ = 2048
INNER = 4096
GN = 1024
DOCS = 2
DOC_MOST = 1536
N_TP = 4


def draw_step_raw(key, part):
    first_key = jax.random.fold_in(key, 11)
    second_key = jax.random.fold_in(key, 12)
    blocks = SEQ // TOK_DEV
    base = jnp.clip(jax.random.normal(first_key, (HEADS, SEQ), jnp.float32), -3.0, 3.0)
    offset = jax.random.uniform(second_key, (HEADS, blocks, 1), jnp.float32, -1.5, 1.5)
    return (base.reshape(HEADS, blocks, TOK_DEV) + offset).reshape(HEADS, SEQ).astype(jnp.bfloat16)


def draw_decay_rate(key, part):
    pick_key = jax.random.fold_in(key, 21)
    slow_key = jax.random.fold_in(key, 22)
    quick_key = jax.random.fold_in(key, 23)
    order = jax.random.permutation(pick_key, HEADS)
    quick_heads = order < HEADS // 2
    slow = jnp.exp(jax.random.uniform(slow_key, (HEADS,), jnp.float32, math.log(0.05), math.log(0.5))) / SEQ
    quick = jnp.exp(jax.random.uniform(quick_key, (HEADS,), jnp.float32, math.log(0.03), math.log(0.1)))
    return jnp.where(quick_heads, quick, slow).astype(jnp.float32)


def draw_decay_jump(key, part):
    spots_key = jax.random.fold_in(key, 31)
    depth_key = jax.random.fold_in(key, 32)
    spots = jax.random.randint(spots_key, (HEADS, 4, 1), 0, SEQ)
    positions = jnp.arange(SEQ, dtype=jnp.int32)
    hit_mask = jnp.any(spots == positions[None, None, :], axis=1)
    depth = jnp.log(jax.random.uniform(depth_key, (HEADS, SEQ), jnp.float32, 0.5, 0.8))
    return jnp.where(hit_mask, depth, 0.0).astype(jnp.float32)


def block_scale(own_key, extent, split, least, high):
    loudness = 1.0
    for axis_at, blocks in split:
        steps = jax.random.uniform(jax.random.fold_in(jax.random.fold_in(own_key, 6), axis_at), (blocks,), jnp.float32, least / len(split), high / len(split))
        loudness = loudness * jnp.repeat(jnp.exp(steps), extent[axis_at] // blocks).reshape((-1,) + (1,) * (len(extent) - 1 - axis_at))
    return loudness


def split_up(amount, total, most, slope):
    loads = [(1 << 20) // math.isqrt(standing ** slope) + 1 for standing in range(2, amount + 1)]
    surplus, counts = total - most - (amount - 1), [1] * (amount - 1)
    while surplus > 0:
        free = [i for i in range(amount - 1) if counts[i] < most]
        whole, left = sum([loads[i] for i in free]), surplus
        for i in free:
            addition = min(most - counts[i], max(1, left * loads[i] // whole), surplus)
            counts[i] = counts[i] + addition
            surplus = surplus - addition
    return np.array([most] + counts)


def uneven(key, count, total, most, skew):
    if count == 2:
        one = jax.random.randint(key, (), max(1, total - most), min(most, total - 1) + 1)
        return jnp.stack([one, total - one])
    lengths = jnp.asarray(split_up(count, total, most, skew), jnp.int32)
    pairs = (count - 1) // 2
    donor, taker = lengths[1:1 + 2 * pairs:2], lengths[2:2 + 2 * pairs:2]
    margin = jnp.minimum(donor - 1, most - taker)
    shifted = jax.random.randint(jax.random.fold_in(key, 1), (pairs,), 0, 1 << 20) % (margin + 1)
    lengths = lengths.at[1:1 + 2 * pairs:2].set(donor - shifted).at[2:2 + 2 * pairs:2].set(taker + shifted)
    return lengths[jax.random.permutation(jax.random.fold_in(key, 2), count)]


def gaussian(rng, extent, scale, limit, split=(), kind=jnp.bfloat16):
    entries = jax.random.normal(rng, extent, jnp.float32) * scale
    if len(split) > 0:
        entries = block_scale(rng, extent, split, -0.22, 0.18) * entries
    return jnp.clip(entries, min=-limit, max=limit).astype(kind)


def setup_inputs(seed: int = 0, part: int = 0) -> dict:
    arg_keys = jax.random.split(jax.random.key(seed), 19)
    own_keys = jax.random.split(jax.random.fold_in(arg_keys[18], part), 19)
    residual = gaussian(own_keys[0], (SEQ, D), 1.0, 6.0, ((0, 4),))
    values = gaussian(own_keys[1], (SEQ, INNER), 1.0, 6.0, ((0, 4), (1, 4)))
    out_gate = gaussian(own_keys[2], (SEQ, INNER), 1.0, 6.0, ((0, 4), (1, 4)))
    writes = gaussian(own_keys[3], (SEQ, GN), 1.0, 6.0, ((0, 4), (1, 4)))
    reads = gaussian(own_keys[4], (SEQ, GN), 1.0, 6.0, ((0, 4), (1, 4)))
    step_raw = draw_step_raw(jax.random.fold_in(jax.random.fold_in(arg_keys[18], part), 71), part)
    decay_rate = draw_decay_rate(jax.random.fold_in(arg_keys[18], 71), part)
    decay_jump = draw_decay_jump(jax.random.fold_in(jax.random.fold_in(arg_keys[18], part), 71), part)
    documents = jnp.searchsorted(jnp.cumsum(uneven(own_keys[8], DOCS, SEQ, DOC_MOST, 0)), jnp.arange(SEQ), side="right").astype(jnp.int32)
    taps_values = gaussian(arg_keys[9], (CONV, INNER), CONV ** -0.5, 3.0, ((1, 4),))
    taps_write = gaussian(arg_keys[10], (CONV, GN), CONV ** -0.5, 3.0, ((1, 4),))
    taps_read = gaussian(arg_keys[11], (CONV, GN), CONV ** -0.5, 3.0, ((1, 4),))
    mixer_gain = jnp.clip(1.0 + 0.18 * jax.random.normal(arg_keys[12], (INNER,), jnp.float32), 0.099609375, 1.8984375).astype(jnp.bfloat16)
    mixer_out = gaussian(arg_keys[13], (INNER, D), INNER ** -0.5, 0.09375, ((0, 4),))
    channel_gain = jnp.clip(1.0 + 0.18 * jax.random.normal(arg_keys[14], (D,), jnp.float32), 0.099609375, 1.8984375).astype(jnp.bfloat16)
    gate_weight = gaussian(arg_keys[15], (D, FF), D ** -0.5, 0.125, ((0, 4), (1, 4)))
    up_weight = gaussian(arg_keys[16], (D, FF), D ** -0.5, 0.125, ((0, 4), (1, 4)))
    down_rows = gaussian(arg_keys[17], (D, FF), FF ** -0.5, 0.078125, ((0, 4), (1, 4)))
    return dict(residual=residual, values=values, out_gate=out_gate, writes=writes, reads=reads, step_raw=step_raw, decay_rate=decay_rate, decay_jump=decay_jump, documents=documents, taps_values=taps_values, taps_write=taps_write, taps_read=taps_read, mixer_gain=mixer_gain, mixer_out=mixer_out, channel_gain=channel_gain, gate_weight=gate_weight, up_weight=up_weight, down_rows=down_rows)


norm_eps = 1e-06

def short_filter(rows, row_docs, taps):
    width = taps.shape[0]
    count = rows.shape[0] - width + 1
    own_docs = row_docs[width - 1:]
    total = jnp.zeros((count, rows.shape[1]), jnp.float32)
    for offset in range(width):
        alive = (row_docs[offset:offset + count] == own_docs).astype(jnp.float32)
        total = total + rows[offset:offset + count].astype(jnp.float32) * taps[offset].astype(jnp.float32)[None, :] * alive[:, None]
    return jax.nn.silu(total).astype(jnp.bfloat16)

def block_pieces(values, writes, reads, step_size, log_decay, segment, heads_per, block):
    span = values.shape[0]
    block_count = span // block
    heads = step_size.shape[0]
    groups = heads // heads_per
    head_size = values.shape[1] // heads
    state_size = writes.shape[1] // groups
    value_blocks = values.astype(jnp.float32).reshape(block_count, block, groups, heads_per, head_size)
    write_blocks = writes.astype(jnp.float32).reshape(block_count, block, groups, state_size)
    read_blocks = reads.astype(jnp.float32).reshape(block_count, block, groups, state_size)
    block_docs = segment.reshape(block_count, block)
    step_blocks = step_size.reshape(groups, heads_per, block_count, block)
    running = jnp.cumsum(log_decay.reshape(groups, heads_per, block_count, block), axis=3)
    target = lax.broadcasted_iota(jnp.int32, (block, block), 0)
    source = lax.broadcasted_iota(jnp.int32, (block, block), 1)
    allowed = (target >= source)[None] & (block_docs[:, :, None] == block_docs[:, None, :])
    scores = jnp.einsum('kign,kjgn->gkij', read_blocks, write_blocks, precision=lax.Precision.HIGHEST)
    spread = running[..., :, None] - running[..., None, :]
    decay = jnp.exp(jnp.where(allowed[None, None], spread, -jnp.inf))
    weights = (decay * scores[:, None] * step_blocks[..., None, :]).astype(jnp.bfloat16)
    inner = jnp.einsum('gekij,kjgep->kigep', weights.astype(jnp.float32), value_blocks, precision=lax.Precision.HIGHEST)
    last_total = running[..., -1]
    same_end = (block_docs == block_docs[:, -1:]).astype(jnp.float32)
    end_factor = jnp.exp(last_total[..., None] - running) * step_blocks * same_end[None, None]
    scaled = (value_blocks * jnp.transpose(end_factor, (2, 3, 0, 1))[..., None]).astype(jnp.bfloat16)
    states = jnp.einsum('kjgep,kjgn->kgepn', scaled.astype(jnp.float32), write_blocks, precision=lax.Precision.HIGHEST)
    return (inner, states, last_total, running, block_docs)

def block_passing(last_total, block_docs, prior_docs):
    return jnp.exp(last_total) * (block_docs[:, -1] == prior_docs).astype(jnp.float32)[None, None]

def carry_states(states, passing, start):

    def advance(held, entry):
        factor, fresh = entry
        return (factor[..., None, None] * held + fresh, held)
    final, entering = lax.scan(advance, start, (jnp.moveaxis(passing, 2, 0), states))
    return (entering, final)

def read_states(reads, entering, running, block_docs, prior_docs):
    block_count, block = block_docs.shape
    groups = entering.shape[1]
    read_blocks = reads.astype(jnp.float32).reshape(block_count, block, groups, -1)
    alive = (block_docs == prior_docs[:, None]).astype(jnp.float32)
    reach = jnp.exp(running) * alive[None, None]
    taken = jnp.einsum('kign,kgepn->kigep', read_blocks, entering, precision=lax.Precision.HIGHEST)
    return taken * jnp.transpose(reach, (2, 3, 0, 1))[..., None]

def sliced_product(left, right_rows, slices):
    width = left.shape[1] // slices
    total = jnp.zeros((left.shape[0], right_rows.shape[0]), jnp.float32)
    for slice_index in range(slices):
        piece = left[:, slice_index * width:(slice_index + 1) * width]
        other = right_rows[:, slice_index * width:(slice_index + 1) * width]
        term = jnp.dot(piece, other.T, preferred_element_type=jnp.float32).astype(jnp.bfloat16)
        term = lax.optimization_barrier(term)
        total = total + term.astype(jnp.float32)
    return total

def reference(residual, values, out_gate, writes, reads, step_raw, decay_rate, decay_jump, documents, taps_values, taps_write, taps_read, mixer_gain, mixer_out, channel_gain, gate_weight, up_weight, down_rows):
    edge = CONV - 1
    segment = documents.astype(jnp.float32)
    row_docs = jnp.concatenate([jnp.full((edge,), -1.0, jnp.float32), segment])

    def padded(rows):
        return jnp.concatenate([jnp.zeros((edge, rows.shape[1]), rows.dtype), rows])
    short_values = short_filter(padded(values), row_docs, taps_values)
    short_writes = short_filter(padded(writes), row_docs, taps_write)
    short_reads = short_filter(padded(reads), row_docs, taps_read)
    step_size = jax.nn.softplus(step_raw.astype(jnp.float32))
    log_decay = decay_jump - decay_rate[:, None] * step_size
    heads_per = HEADS // GROUPS

    def advance(carry, index):
        held, prior = carry
        first = index * BLOCK
        reads_here = lax.dynamic_slice_in_dim(short_reads, first, BLOCK, 0)
        inner, states, last_total, running, block_docs = block_pieces(lax.dynamic_slice_in_dim(short_values, first, BLOCK, 0), lax.dynamic_slice_in_dim(short_writes, first, BLOCK, 0), reads_here, lax.dynamic_slice_in_dim(step_size, first, BLOCK, 1), lax.dynamic_slice_in_dim(log_decay, first, BLOCK, 1), lax.dynamic_slice_in_dim(segment, first, BLOCK, 0), heads_per, BLOCK)
        prior_docs = prior.reshape(1)
        passing = block_passing(last_total, block_docs, prior_docs)
        entering, final = carry_states(states, passing, held)
        mixed = inner + read_states(reads_here, entering, running, block_docs, prior_docs)
        return ((final, block_docs[0, -1]), mixed.reshape(BLOCK, INNER))
    start_state = jnp.zeros((GROUPS, heads_per, HDIM, STATE), jnp.float32)
    start_doc = jnp.asarray(-1.0, jnp.float32)
    indices = jnp.arange(SEQ // BLOCK, dtype=jnp.int32)
    _, outputs = lax.scan(advance, (start_state, start_doc), indices)
    mixed = outputs.reshape(SEQ, INNER)
    gated = mixed * jax.nn.silu(out_gate.astype(jnp.float32))
    grouped = gated.reshape(SEQ, GROUPS, INNER // GROUPS)
    grouped = grouped * lax.rsqrt(lax.optimization_barrier(jnp.mean(grouped * grouped, axis=2, keepdims=True)) + norm_eps)
    mixer_in = (grouped.reshape(SEQ, INNER) * mixer_gain.astype(jnp.float32)[None, :]).astype(jnp.bfloat16)
    mix = sliced_product(mixer_in, mixer_out.T, N_TP)
    after = (residual.astype(jnp.float32) + mix).astype(jnp.bfloat16)
    after_wide = after.astype(jnp.float32)
    normal = after_wide * lax.rsqrt(lax.optimization_barrier(jnp.mean(after_wide * after_wide, axis=1, keepdims=True)) + norm_eps)
    normal = (normal * channel_gain.astype(jnp.float32)[None, :]).astype(jnp.bfloat16)
    gate = jnp.dot(normal, gate_weight, preferred_element_type=jnp.float32)
    up = jnp.dot(normal, up_weight, preferred_element_type=jnp.float32)
    hidden = (jax.nn.silu(gate) * up).astype(jnp.bfloat16)
    down = sliced_product(hidden, down_rows, N_TP)
    return (after.astype(jnp.float32) + down).astype(jnp.bfloat16)
```

```python
import functools

import jax
import jax.numpy as jnp
from jax import lax
from jax.experimental import pallas as pl
from jax.experimental.pallas import tpu as pltpu
from jax.sharding import PartitionSpec as P


MESH = pl.DeviceIdType.MESH

HEADS = 64
GROUPS = 8
BLOCK = 128


norm_eps = 1e-06


def from_behind(value, axis, by):
    peers = lax.axis_size(axis)
    pairs = [(i, i + by) for i in range(peers) if 0 <= i + by < peers]
    return lax.ppermute(value, axis, pairs)


def entering_state(decay, state, first_doc, last_doc, axis):
    peers, index = (lax.axis_size(axis), lax.axis_index(axis))
    heads = decay.size
    lanes = state.shape[-1]
    marks = jnp.concatenate([decay.reshape(-1), first_doc, last_doc])
    marks = jnp.pad(marks, (0, lanes - heads - 2))
    rows = jnp.broadcast_to(marks[None], (16, lanes))
    packed = jnp.concatenate([state.reshape(-1, lanes), rows]).astype(jnp.bfloat16)
    held = jnp.zeros(state.shape, jnp.float32)
    factor = jnp.ones((heads,), jnp.float32)
    before = jnp.full((1,), -1.0, jnp.float32)
    later_first = None
    for k in range(1, peers):
        there = k <= index
        got = from_behind(packed, axis, k)
        marks = got[-1].astype(jnp.float32)
        if k == 1:
            before = jnp.where(there, marks[heads + 1 : heads + 2], before)
        else:
            factor = factor * (later_first == marks[heads + 1])
        weight = jnp.where(there, factor, 0.0).reshape(decay.shape)
        part = got[:-16].astype(jnp.float32).reshape(state.shape)
        held = held + weight[..., None, None] * part
        factor = factor * marks[:heads]
        later_first = marks[heads]
    return held, before


def short_filter(rows, row_docs, taps):
    width = taps.shape[0]
    count = rows.shape[0] - width + 1
    own_docs = row_docs[width - 1 :]
    total = jnp.zeros((count, rows.shape[1]), jnp.float32)
    for offset in range(width):
        alive = (row_docs[offset : offset + count] == own_docs).astype(jnp.float32)
        total = (
            total
            + rows[offset : offset + count].astype(jnp.float32)
            * taps[offset].astype(jnp.float32)[None, :]
            * alive[:, None]
        )
    return jax.nn.silu(total).astype(jnp.bfloat16)


def block_pieces(values, writes, reads, step_size, log_decay, segment, heads_per, block):
    span = values.shape[0]
    block_count = span // block
    heads = step_size.shape[0]
    groups = heads // heads_per
    head_size = values.shape[1] // heads
    state_size = writes.shape[1] // groups
    value_blocks = values.reshape(block_count, block, groups, heads_per, head_size)
    write_blocks = writes.reshape(block_count, block, groups, state_size)
    read_blocks = reads.reshape(block_count, block, groups, state_size)
    block_docs = segment.reshape(block_count, block)
    step_blocks = step_size.reshape(groups, heads_per, block_count, block)
    running = jnp.cumsum(log_decay.reshape(groups, heads_per, block_count, block), axis=3)
    target = lax.broadcasted_iota(jnp.int32, (block, block), 0)
    source = lax.broadcasted_iota(jnp.int32, (block, block), 1)
    allowed = (target >= source)[None] & (block_docs[:, :, None] == block_docs[:, None, :])
    scores = jnp.einsum(
        "kign,kjgn->gkij", read_blocks, write_blocks, preferred_element_type=jnp.float32
    )
    spread = running[..., :, None] - running[..., None, :]
    decay = jnp.exp(jnp.where(allowed[None, None], spread, -jnp.inf))
    weights = (decay * scores[:, None] * step_blocks[..., None, :]).astype(jnp.bfloat16)
    inner = jnp.einsum(
        "gekij,kjgep->kigep", weights, value_blocks, preferred_element_type=jnp.float32
    )
    last_total = running[..., -1]
    same_end = (block_docs == block_docs[:, -1:]).astype(jnp.float32)
    end_factor = jnp.exp(last_total[..., None] - running) * step_blocks * same_end[None, None]
    scaled = (
        value_blocks.astype(jnp.float32) * jnp.transpose(end_factor, (2, 3, 0, 1))[..., None]
    ).astype(jnp.bfloat16)
    states = jnp.einsum(
        "kjgep,kjgn->kgepn", scaled, write_blocks, preferred_element_type=jnp.float32
    )
    return (inner, states, last_total, running, block_docs)


def block_passing(last_total, block_docs, prior_docs):
    return jnp.exp(last_total) * (block_docs[:, -1] == prior_docs).astype(jnp.float32)[None, None]


def carry_states(states, passing, start):

    def advance(held, entry):
        factor, fresh = entry
        return (factor[..., None, None] * held + fresh, held)

    final, entering = lax.scan(advance, start, (jnp.moveaxis(passing, 2, 0), states))
    return (entering, final)


def read_states(reads, entering, running, block_docs, prior_docs):
    block_count, block = block_docs.shape
    groups = entering.shape[1]
    read_blocks = reads.astype(jnp.float32).reshape(block_count, block, groups, -1)
    alive = (block_docs == prior_docs[:, None]).astype(jnp.float32)
    reach = jnp.exp(running) * alive[None, None]
    taken = jnp.einsum("kign,kgepn->kigep", read_blocks, entering, precision=lax.Precision.HIGHEST)
    return taken * jnp.transpose(reach, (2, 3, 0, 1))[..., None]


def down_product(hidden, rows):
    return lax.dot_general(
        hidden, rows, (((1,), (1,)), ((), ())), preferred_element_type=jnp.float32
    )


def greet(peers, me):
    barrier = pltpu.get_barrier_semaphore()
    for off in range(1, peers):
        pl.semaphore_signal(
            barrier, inc=1, device_id={"tp": lax.rem(me + off, peers)}, device_id_type=MESH
        )
    pl.semaphore_wait(barrier, peers - 1)


def tp_copy(src, dst, send, recv, peer):
    return pltpu.make_async_remote_copy(
        src_ref=src,
        dst_ref=dst,
        send_sem=send,
        recv_sem=recv,
        device_id={"tp": peer},
        device_id_type=MESH,
    )


def columns_of(index, share):
    return pl.ds(pl.multiple_of(index * share, share), share)


def mix_kernel(
    peers, mixer_ref, out_ref, res_ref, gain_ref, own_ref, normal_ref,
    going, coming, own_part, shared, sums, send_a, recv_a, send_b, recv_b,
):
    me = lax.axis_index("tp")
    share = own_part.shape[1]
    greet(peers, me)
    copies = []
    for off in range(peers - 1, 0, -1):
        peer = lax.rem(me + off, peers)
        going[off - 1] = jnp.dot(
            mixer_ref[...], out_ref[:, columns_of(peer, share)], preferred_element_type=jnp.float32
        ).astype(jnp.bfloat16)
        copy = tp_copy(
            going.at[off - 1], coming.at[off - 1], send_a.at[off - 1], recv_a.at[off - 1], peer
        )
        copy.start()
        copies.append(copy)
    mine = columns_of(me, share)
    total = (
        jnp.dot(mixer_ref[...], out_ref[:, mine], preferred_element_type=jnp.float32)
        .astype(jnp.bfloat16)
        .astype(jnp.float32)
    )
    for copy in copies:
        copy.wait_recv()
    for off in range(1, peers):
        total = total + coming[off - 1].astype(jnp.float32)
    after = (res_ref[:, mine].astype(jnp.float32) + total).astype(jnp.bfloat16)
    own_part[...] = after
    own_ref[...] = after
    later = []
    for off in range(peers - 1, 0, -1):
        copy = tp_copy(
            own_part, shared.at[off - 1], send_b.at[off - 1], recv_b.at[off - 1],
            lax.rem(me + off, peers),
        )
        copy.start()
        later.append(copy)
    wide = after.astype(jnp.float32)
    squares = jnp.sum(wide * wide, axis=1, keepdims=True)
    for copy in later:
        copy.wait_recv()
    for off in range(1, peers):
        wide = shared[off - 1].astype(jnp.float32)
        squares = squares + jnp.sum(wide * wide, axis=1, keepdims=True)
    scale = lax.rsqrt(squares / (share * peers) + norm_eps)
    normal_ref[:, mine] = (
        own_part[...].astype(jnp.float32) * scale * gain_ref[:, mine].astype(jnp.float32)
    ).astype(jnp.bfloat16)
    for off in range(1, peers):
        theirs = columns_of(lax.rem(me - off + peers, peers), share)
        normal_ref[:, theirs] = (
            shared[off - 1].astype(jnp.float32) * scale * gain_ref[:, theirs].astype(jnp.float32)
        ).astype(jnp.bfloat16)
    for copy in copies + later:
        copy.wait_send()


def mix_and_norm(mixer_in, mixer_out, residual, channel_gain):
    peers = lax.axis_size("tp")
    rows, width = residual.shape
    share = width // peers
    flops = 2 * rows * width * mixer_in.shape[1]
    part = (peers - 1, rows, share)
    return pl.pallas_call(
    functools.partial(mix_kernel, peers),
    out_shape=(
        jax.ShapeDtypeStruct((rows, share), jnp.bfloat16),
        jax.ShapeDtypeStruct((rows, width), jnp.bfloat16),
    ),
    in_specs=[pl.BlockSpec(memory_space=pltpu.VMEM)] * 4,
    out_specs=[pl.BlockSpec(memory_space=pltpu.VMEM)] * 2,
    scratch_shapes=[
        pltpu.VMEM(part, jnp.bfloat16),
        pltpu.VMEM(part, jnp.bfloat16),
        pltpu.VMEM((rows, share), jnp.bfloat16),
        pltpu.VMEM(part, jnp.bfloat16),
        pltpu.VMEM((rows, 128), jnp.float32),
    ]
    + [pltpu.SemaphoreType.DMA((peers - 1,))] * 4,
    compiler_params=pltpu.CompilerParams(
        collective_id=0, has_side_effects=True, vmem_limit_bytes=40 * 1024 * 1024
    ),
    cost_estimate=pl.CostEstimate(flops=20 * flops, bytes_accessed=0, transcendentals=0),
    name="mix_and_norm",
    )(mixer_in, mixer_out, residual, channel_gain.reshape(1, width))


def down_kernel(peers, part_ref, result_ref, coming, send_a, recv_a):
    me = lax.axis_index("tp")
    greet(peers, me)
    copies = []
    for off in range(peers - 1, 0, -1):
        peer = lax.rem(me + off, peers)
        copy = tp_copy(
            part_ref.at[peer], coming.at[off - 1], send_a.at[off - 1], recv_a.at[off - 1], peer
        )
        copy.start()
        copies.append(copy)
    total = part_ref[me].astype(jnp.float32)
    for copy in copies:
        copy.wait_recv()
    for off in range(1, peers):
        total = total + coming[off - 1].astype(jnp.float32)
    result_ref[...] = total
    for copy in copies:
        copy.wait_send()


def add_down(parts, place):
    peers, rows, share = parts.shape
    return pl.pallas_call(
        functools.partial(down_kernel, peers),
        out_shape=jax.ShapeDtypeStruct((rows, share), jnp.float32),
        in_specs=[pl.BlockSpec(memory_space=pltpu.VMEM)],
        out_specs=pl.BlockSpec(memory_space=pltpu.VMEM),
        scratch_shapes=[pltpu.VMEM((peers - 1, rows, share), jnp.bfloat16)]
        + [pltpu.SemaphoreType.DMA((peers - 1,))] * 2,
        compiler_params=pltpu.CompilerParams(collective_id=place, has_side_effects=True),
    )(parts)


def gather_weights(weights):
    first = lax.axis_index("grp")
    columns = weights[0].shape[1]
    half = -(-columns // 256) * 128
    rest = columns - half
    near, local = [], []
    rows = weights[2].shape[0] // 2
    pieces = (weights[0], weights[1], weights[2][:rows], weights[2][rows:])
    for weight in pieces:
        piece = lax.dynamic_slice_in_dim(weight, first * rest, half, 1)
        near.append(lax.all_gather(piece, "sp", axis=0))
        local.append(lax.dynamic_slice_in_dim(weight, (1 - first) * half, rest, 1))
    return near, local


def swap(gathered, columns):
    steps, rows, half = gathered.shape
    index, first = (lax.axis_index("sp"), lax.axis_index("grp"))
    lead = first * (2 * half - columns)
    turn = [
        lax.dynamic_slice(
            gathered, (lax.rem(index + k, steps), 0, lead), (1, rows, columns - half)
        )
        for k in range(1, steps)
    ]
    return lax.ppermute(jnp.concatenate(turn).reshape(-1, columns - half), "grp", [(0, 1), (1, 0)])


def turned(array, by):
    return lax.dynamic_slice_in_dim(
        jnp.concatenate([array, array], axis=1), by, array.shape[1], 1
    )


def channel_mixer(normal, own_after, near, local, far):
    tokens, _ = normal.shape
    rows = local[0].shape[0]
    half = near[0].shape[2]
    here = lax.axis_index("sp") * rows
    mine = turned(normal, here)

    def product(k):
        return jnp.dot(
            mine[:, :rows], local[k], preferred_element_type=jnp.float32
        ) + jnp.dot(mine[:, rows:], far[k], preferred_element_type=jnp.float32)

    whole = [weight.reshape(-1, weight.shape[2]) for weight in near]
    gate = jnp.dot(normal, whole[0], preferred_element_type=jnp.float32)
    up = jnp.dot(normal, whole[1], preferred_element_type=jnp.float32)
    hidden = (jax.nn.silu(gate) * up).astype(jnp.bfloat16)
    columns = half + far[0].shape[1]
    late, hidden = lax.optimization_barrier((near[2], hidden))
    far_low = swap(late, columns)
    last, far_low = lax.optimization_barrier((near[3], far_low))
    far_high = swap(last, columns)
    others = (jax.nn.silu(product(0)) * product(1)).astype(jnp.bfloat16)

    def down_part(here_rows, gathered, swapped, kept, name):
        steps, count, _ = gathered.shape
        down_near = down_product(hidden, gathered.reshape(-1, half))
        down_far = jnp.concatenate(
            [down_product(others, kept), down_product(others, swapped)], axis=1
        )
        down = down_near + turned(down_far, steps * count - here_rows)
        peers = lax.axis_size("tp")
        share = steps * count // peers
        parts = jnp.stack(
            [down[:, k * share : (k + 1) * share].astype(jnp.bfloat16) for k in range(peers)]
        )
        return add_down(parts, name).reshape(tokens, -1, count)

    low = down_part(here // 2, late, far_low, local[2], 1)
    high = down_part(here // 2, last, far_high, local[3], 2)
    down = jnp.concatenate([low, high], axis=2).reshape(own_after.shape)
    return (own_after.astype(jnp.float32) + down).astype(jnp.bfloat16)


def on_device(
    residual,
    values,
    out_gate,
    writes,
    reads,
    step_raw,
    decay_rate,
    decay_jump,
    documents,
    taps_values,
    taps_write,
    taps_read,
    mixer_gain,
    mixer_out,
    channel_gain,
    gate_weight,
    up_weight,
    down_rows,
):
    near, local = gather_weights((gate_weight, up_weight, down_rows))
    tokens = values.shape[0]
    edge = taps_values.shape[0] - 1
    segment = documents.astype(jnp.float32)
    wide, narrow = values.shape[1], writes.shape[1]
    tail_docs = jnp.broadcast_to(segment[tokens - edge :, None], (edge, 128)).astype(jnp.bfloat16)
    behind = from_behind(
        jnp.concatenate(
            [values[tokens - edge :], writes[tokens - edge :], reads[tokens - edge :], tail_docs],
            axis=1,
        ),
        "sp",
        1,
    )
    before = (
        behind[:, :wide],
        behind[:, wide : wide + narrow],
        behind[:, wide + narrow : wide + 2 * narrow],
        behind[:, wide + 2 * narrow],
    )
    row_docs = jnp.concatenate([before[3].astype(jnp.float32), segment])
    short_values = short_filter(jnp.concatenate([before[0], values]), row_docs, taps_values)
    short_writes = short_filter(jnp.concatenate([before[1], writes]), row_docs, taps_write)
    short_reads = short_filter(jnp.concatenate([before[2], reads]), row_docs, taps_read)
    step_size = jax.nn.softplus(step_raw.astype(jnp.float32))
    log_decay = decay_jump - decay_rate[:, None] * step_size
    heads_per = HEADS // GROUPS
    inner, states, last_total, running, block_docs = block_pieces(
        short_values, short_writes, short_reads, step_size, log_decay, segment, heads_per, BLOCK
    )
    groups = states.shape[1]
    local_prior = jnp.concatenate([jnp.full((1,), -1.0, jnp.float32), block_docs[:-1, -1]])
    zero_state = jnp.zeros(states.shape[1:], jnp.float32)
    entering, final = carry_states(
        states, block_passing(last_total, block_docs, local_prior), zero_state
    )
    whole_decay = jnp.exp(jnp.sum(last_total, axis=2)) * (segment[0] == segment[-1]).astype(
        jnp.float32
    )
    held, before_doc = entering_state(whole_decay, final, segment[:1], segment[-1:], "sp")
    early, held = lax.optimization_barrier((near[0], held))
    far_gate = swap(early, gate_weight.shape[1])
    prior_docs = jnp.concatenate([before_doc, block_docs[:-1, -1]])
    passing_in = block_passing(last_total, block_docs, prior_docs)
    gains = jnp.cumprod(passing_in, axis=2)
    gains = jnp.concatenate([jnp.ones_like(gains[..., :1]), gains[..., :-1]], axis=2)
    entering = entering + jnp.moveaxis(gains, 2, 0)[..., None, None] * held[None]
    mixed = inner + read_states(short_reads, entering, running, block_docs, prior_docs)
    gated = mixed.reshape(tokens, -1) * jax.nn.silu(out_gate.astype(jnp.float32))
    grouped = gated.reshape(tokens, groups, -1)
    grouped = grouped * lax.rsqrt(jnp.mean(grouped * grouped, axis=2, keepdims=True) + norm_eps)
    mixer_in = (grouped.reshape(tokens, -1) * mixer_gain.astype(jnp.float32)[None, :]).astype(
        jnp.bfloat16
    )
    own_after, normal = mix_and_norm(mixer_in, mixer_out, residual, channel_gain)
    middle, far_gate, normal = lax.optimization_barrier((near[1], far_gate, normal))
    far_up = swap(middle, gate_weight.shape[1])
    return channel_mixer(normal, own_after, near, local, (far_gate, far_up))


def solution(mesh):
    return jax.shard_map(
        on_device,
        mesh=mesh,
        in_specs=(
            P(("grp", "sp"), None),
            P(("grp", "sp"), "tp"),
            P(("grp", "sp"), "tp"),
            P(("grp", "sp"), "tp"),
            P(("grp", "sp"), "tp"),
            P("tp", ("grp", "sp")),
            P("tp"),
            P("tp", ("grp", "sp")),
            P(("grp", "sp")),
            P(None, "tp"),
            P(None, "tp"),
            P(None, "tp"),
            P("tp"),
            P("tp", None),
            P(),
            P("sp", "tp"),
            P("sp", "tp"),
            P("sp", "tp"),
        ),
        out_specs=P(("grp", "sp"), "tp"),
        check_vma=False,
    )
```
